32 devices in a mesh: sp: 8 (over z, y), tp: 4 (over x, core).
Axes of the slice: x: 2, y: 2, z: 4, core: 2. Of those that a mesh axis runs over, the one named last changes fastest.
Arguments:
- resid: bfloat16 [2048, 2048], P(('sp', 'tp')), may hold values from -0.3125 to 0.3125
- q_latent: bfloat16 [2048, 768], P('sp'), may hold values from -6 to 6
- kv_latent: bfloat16 [2048, 512], P('sp'), may hold values from -6 to 6
- rope_key: bfloat16 [2048, 32], P('sp'), may hold values from -6 to 6
- q_gain: float32 [768], replicated, may hold values from 0.6 to 10, as said below
- kv_gain: float32 [512], replicated, may hold values from 0.6 to 10
- w_q_small: bfloat16 [768, 768], P(None, 'tp'), may hold values from -0.21875 to 0.21875
- w_q_large: bfloat16 [768, 1280], P(None, 'tp'), may hold values from -0.21875 to 0.21875
- w_kv_small: bfloat16 [512, 1024], P(None, 'tp'), may hold values from -0.25 to 0.25
- w_kv_large: bfloat16 [512, 2048], P(None, 'tp'), may hold values from -0.25 to 0.25
- w_out_small: bfloat16 [512, 2048], P('tp'), may hold values from -0.15625 to 0.15625
- w_out_large: bfloat16 [1024, 2048], P('tp'), may hold values from -0.15625 to 0.15625
- ffn_gain: float32 [2048], replicated, may hold values from 0.1 to 1.9
- w_up: bfloat16 [2048, 8192], P('sp', 'tp'), may hold values from -0.125 to 0.125
- w_down: bfloat16 [8192, 2048], P('tp', 'sp'), may hold values from -0.0625 to 0.0625
Outputs:
- layer_out: bfloat16 [2048, 2048], P(('sp', 'tp'))
The draws below stay inside these ranges and needn't reach their ends.
Inputs may be any that keep to these rules, and one draw needn't show every extreme that they name: q_gain and kv_gain are positive.
All inputs are finite; a program needn't handle non-finite values.
Results may differ from the reference program's by a relative error of at most 0.025.
The reference program's roundings to bfloat16 on the way (of `query_normed`, `key_normed`, `key_rot`, `weights`, `after_attn`, `ffn_normed` and `hidden`) count: a program that leaves them out, or rounds other values in their place, can miss the bound.
Values may be sent and summed in bfloat16 or wider, within the bound.
A program may use at most 128 MiB of HBM per device.

```python
import math
import jax
import jax.numpy as jnp
from jax import lax

WIDTH = 2048
MIXER_UNITS = 8192
QUERY_RANK = 768
LATENT_RANK = 512
HEADS_SMALL = 8
HEADS_LARGE = 8
SMALL_DIM = 64
LARGE_DIM = 128
ROPE_DIM = 32
TOKENS = 2048


def draw_q_gain(key, part):
    return jnp.exp(jax.random.uniform(key, (QUERY_RANK,), jnp.float32, -0.4, 0.4))


def draw_kv_gain(key, part):
    return jnp.exp(jax.random.uniform(key, (LATENT_RANK,), jnp.float32, -0.4, 0.4))


def block_levels(own_key, shape, shards, low, largest):
    factor_of, own = 1.0, jax.random.fold_in(own_key, 6)
    for position, shards_of in shards:
        heights = jnp.exp(jax.random.uniform(jax.random.fold_in(own, position), (shards_of,), jnp.float32, low / len(shards), largest / len(shards)))
        factor_of = factor_of * jnp.repeat(heights, shape[position] // shards_of).reshape([-1 if axis == position else 1 for axis in range(len(shape))])
    return factor_of


def normal_values(own_key, dims, width, limit, cuts=(), held_as=jnp.bfloat16):
    values = width * jax.random.normal(own_key, dims, jnp.float32)
    if cuts:
        values = values * block_levels(own_key, dims, cuts, -0.22, 0.18)
    return jnp.clip(values, -limit, limit).astype(held_as)


def setup_inputs(seed: int = 0) -> dict:
    arg_keys = jax.random.split(jax.random.key(seed), 16)
    return {
        "resid": normal_values(arg_keys[0], (TOKENS, WIDTH), 0.02, 0.3125, ((0, 32),)),
        "q_latent": normal_values(arg_keys[1], (TOKENS, QUERY_RANK), 1.0, 6.0, ((0, 8),)),
        "kv_latent": normal_values(arg_keys[2], (TOKENS, LATENT_RANK), 1.0, 6.0, ((0, 8),)),
        "rope_key": normal_values(arg_keys[3], (TOKENS, ROPE_DIM), 1.0, 6.0, ((0, 8),)),
        "q_gain": draw_q_gain(jax.random.fold_in(arg_keys[15], 71), 0),
        "kv_gain": draw_kv_gain(jax.random.fold_in(arg_keys[15], 71), 0),
        "w_q_small": normal_values(arg_keys[6], (QUERY_RANK, HEADS_SMALL * (SMALL_DIM + ROPE_DIM)), QUERY_RANK ** -0.5, 0.21875, ((1, 4),)),
        "w_q_large": normal_values(arg_keys[7], (QUERY_RANK, HEADS_LARGE * (LARGE_DIM + ROPE_DIM)), QUERY_RANK ** -0.5, 0.21875, ((1, 4),)),
        "w_kv_small": normal_values(arg_keys[8], (LATENT_RANK, HEADS_SMALL * 2 * SMALL_DIM), LATENT_RANK ** -0.5, 0.25, ((1, 4),)),
        "w_kv_large": normal_values(arg_keys[9], (LATENT_RANK, HEADS_LARGE * 2 * LARGE_DIM), LATENT_RANK ** -0.5, 0.25, ((1, 4),)),
        "w_out_small": normal_values(arg_keys[10], (HEADS_SMALL * SMALL_DIM, WIDTH), (HEADS_SMALL * SMALL_DIM + HEADS_LARGE * LARGE_DIM) ** -0.5, 0.15625, ((0, 4),)),
        "w_out_large": normal_values(arg_keys[11], (HEADS_LARGE * LARGE_DIM, WIDTH), (HEADS_SMALL * SMALL_DIM + HEADS_LARGE * LARGE_DIM) ** -0.5, 0.15625, ((0, 4),)),
        "ffn_gain": jnp.clip(1.0 + 0.18 * jax.random.normal(arg_keys[12], (WIDTH,), jnp.float32), 0.1, 1.9),
        "w_up": normal_values(arg_keys[13], (WIDTH, MIXER_UNITS), WIDTH ** -0.5, 0.125, ((0, 8), (1, 4))),
        "w_down": normal_values(arg_keys[14], (MIXER_UNITS, WIDTH), MIXER_UNITS ** -0.5, 0.0625, ((0, 4), (1, 8))),
    }


epsilon = 1e-06
theta_base = 10000.0

def rms_scale(inputs, gain_vec):
    values = inputs.astype(jnp.float32)
    return values * lax.rsqrt(lax.optimization_barrier(jnp.mean(values * values, axis=-1, keepdims=True)) + epsilon) * gain_vec

def rotary(values, positions):
    halfway = values.shape[-1] // 2
    inverse = theta_base ** (-jnp.arange(0, 2 * halfway, 2, dtype=jnp.float32) / (2 * halfway))
    angles = positions.astype(jnp.float32)[:, None] * inverse[None, :]
    cos_table = jnp.cos(angles)
    sin_table = jnp.sin(angles)
    if values.ndim == 3:
        cos_table = cos_table[:, None, :]
        sin_table = sin_table[:, None, :]
    first_half = values[..., :halfway]
    second_half = values[..., halfway:]
    return jnp.concatenate([first_half * cos_table - second_half * sin_table, second_half * cos_table + first_half * sin_table], axis=-1)

def queries(normed, weight, nope_dim, positions):
    projected = jnp.dot(normed, weight, preferred_element_type=jnp.float32)
    projected = projected.reshape(projected.shape[0], -1, nope_dim + ROPE_DIM)
    turned = rotary(projected[..., nope_dim:], positions)
    return jnp.concatenate([projected[..., :nope_dim], turned], axis=-1).astype(jnp.bfloat16)

def group_attention(query_rows, keys_values, key_rot, nope_dim):
    length = query_rows.shape[0]
    head_count = query_rows.shape[1]
    block_rows = math.gcd(length, 512)
    block_count = length // block_rows
    key_part = keys_values[..., :nope_dim].astype(jnp.float32)
    value_part = keys_values[..., nope_dim:].astype(jnp.float32)
    rot_f32 = key_rot.astype(jnp.float32)
    score_scale = (nope_dim + ROPE_DIM) ** (-0.5)
    key_pos = jnp.arange(length, dtype=jnp.int32)

    def attend_block(block_args):
        query_block, block_index = block_args
        query_f32 = query_block.astype(jnp.float32)
        scores = jnp.einsum('qhd,khd->hqk', query_f32[..., :nope_dim], key_part)
        scores = scores + jnp.einsum('qhr,kr->hqk', query_f32[..., nope_dim:], rot_f32)
        scores = scores * score_scale
        query_pos = block_index * block_rows + jnp.arange(block_rows, dtype=jnp.int32)
        causal = key_pos[None, :] <= query_pos[:, None]
        scores = jnp.where(causal[None], scores, -jnp.inf)
        row_max = lax.optimization_barrier(jnp.max(scores, axis=-1, keepdims=True))
        exponent = jnp.exp(scores - row_max)
        row_sum = lax.optimization_barrier(jnp.sum(exponent, axis=-1))
        weights = lax.optimization_barrier(exponent.astype(jnp.bfloat16)).astype(jnp.float32)
        summed = jnp.einsum('hqk,khd->qhd', weights, value_part)
        return (summed / jnp.transpose(row_sum)[:, :, None]).astype(jnp.bfloat16)
    blocks = query_rows.reshape(block_count, block_rows, head_count, query_rows.shape[-1])
    result = lax.map(attend_block, (blocks, jnp.arange(block_count, dtype=jnp.int32)))
    return result.reshape(length, -1)

def reference(resid, q_latent, kv_latent, rope_key, q_gain, kv_gain, w_q_small, w_q_large, w_kv_small, w_kv_large, w_out_small, w_out_large, ffn_gain, w_up, w_down):
    positions = jnp.arange(TOKENS, dtype=jnp.int32)
    query_normed = rms_scale(q_latent, q_gain).astype(jnp.bfloat16)
    key_normed = rms_scale(kv_latent, kv_gain).astype(jnp.bfloat16)
    key_rot = rotary(rope_key.astype(jnp.float32), positions).astype(jnp.bfloat16)
    query_small = queries(query_normed, w_q_small, SMALL_DIM, positions)
    query_large = queries(query_normed, w_q_large, LARGE_DIM, positions)
    kv_small = jnp.dot(key_normed, w_kv_small, preferred_element_type=jnp.float32).astype(jnp.bfloat16)
    kv_small = kv_small.reshape(TOKENS, HEADS_SMALL, 2 * SMALL_DIM)
    kv_large = jnp.dot(key_normed, w_kv_large, preferred_element_type=jnp.float32).astype(jnp.bfloat16)
    kv_large = kv_large.reshape(TOKENS, HEADS_LARGE, 2 * LARGE_DIM)
    attn_small = group_attention(query_small, kv_small, key_rot, SMALL_DIM)
    attn_large = group_attention(query_large, kv_large, key_rot, LARGE_DIM)
    mixed_rows = jnp.dot(attn_small, w_out_small, preferred_element_type=jnp.float32)
    mixed_rows = mixed_rows + jnp.dot(attn_large, w_out_large, preferred_element_type=jnp.float32)
    after_attn = (resid.astype(jnp.float32) + mixed_rows).astype(jnp.bfloat16)
    ffn_normed = rms_scale(after_attn, ffn_gain).astype(jnp.bfloat16)
    hidden = jnp.square(jax.nn.relu(jnp.dot(ffn_normed, w_up, preferred_element_type=jnp.float32)))
    hidden = hidden.astype(jnp.bfloat16)
    ffn_rows = jnp.dot(hidden, w_down, preferred_element_type=jnp.float32)
    return (after_attn.astype(jnp.float32) + ffn_rows).astype(jnp.bfloat16)
```

```python
import functools
import math

import jax
import jax.numpy as jnp
from jax import lax
from jax.experimental import pallas as pl
from jax.experimental.pallas import tpu as pltpu
from jax.sharding import PartitionSpec as P

SMALL_DIM = 64
LARGE_DIM = 128
ROPE_DIM = 32


epsilon = 1e-06
theta_base = 10000.0
mask_floor = -1e30


def rms_scale(inputs, gain_vec):
    values = inputs.astype(jnp.float32)
    return (
        values * lax.rsqrt(jnp.mean(values * values, axis=-1, keepdims=True) + epsilon) * gain_vec
    )


def rotary(values, positions):
    halfway = values.shape[-1] // 2
    inverse = theta_base ** (-jnp.arange(0, 2 * halfway, 2, dtype=jnp.float32) / (2 * halfway))
    angles = positions.astype(jnp.float32)[:, None] * inverse[None, :]
    cos_table = jnp.cos(angles)
    sin_table = jnp.sin(angles)
    if values.ndim == 3:
        cos_table = cos_table[:, None, :]
        sin_table = sin_table[:, None, :]
    first_half = values[..., :halfway]
    second_half = values[..., halfway:]
    return jnp.concatenate(
        [
            first_half * cos_table - second_half * sin_table,
            second_half * cos_table + first_half * sin_table,
        ],
        axis=-1,
    )


def queries(normed, weight, nope_dim, positions):
    projected = jnp.dot(normed, weight, preferred_element_type=jnp.float32)
    projected = projected.reshape(projected.shape[0], -1, nope_dim + ROPE_DIM)
    turned = rotary(projected[..., nope_dim:], positions)
    return jnp.concatenate([projected[..., :nope_dim], turned], axis=-1).astype(jnp.bfloat16)


def update_group(
    running, query_rows, key_block, value_block, key_rot, query_pos, key_pos, nope_dim
):
    row_max, row_sum, weighted = running
    score_scale = query_rows.shape[-1] ** (-0.5)
    scores = jnp.einsum(
        "qhd,khd->hqk", query_rows[..., :nope_dim], key_block, preferred_element_type=jnp.float32
    )
    scores = scores + jnp.einsum(
        "qhr,kr->hqk", query_rows[..., nope_dim:], key_rot, preferred_element_type=jnp.float32
    )
    scores = scores * score_scale
    causal = (key_pos[None, :] <= query_pos[:, None])[None]
    masked = jnp.where(causal, scores, mask_floor)
    new_max = jnp.maximum(row_max, jnp.max(masked, axis=-1))
    shrink = jnp.exp(row_max - new_max)
    weights = jnp.where(causal, jnp.exp(masked - new_max[..., None]), 0.0)
    row_sum = row_sum * shrink + jnp.sum(weights, axis=-1)
    weighted = weighted * shrink[..., None] + jnp.einsum(
        "hqk,khd->hqd",
        weights.astype(jnp.bfloat16),
        value_block,
        preferred_element_type=jnp.float32,
    )
    return (new_max, row_sum, weighted)


MESH = pl.DeviceIdType.MESH
CORES = 2
LANES = 128


def inner_split(count):
    best = 1
    for size in range(1, count + 1):
        if size * size <= count and count % size == 0:
            best = size
    return best


def remote(src, dst, send_sem, recv_sem, device):
    return pltpu.make_async_remote_copy(
        src_ref=src,
        dst_ref=dst,
        send_sem=send_sem,
        recv_sem=recv_sem,
        device_id=device,
        device_id_type=MESH,
    )


def place(ny, nz, nx):
    s, t = lax.axis_index("sp"), lax.axis_index("tp")
    z, y = s // ny, s % ny
    x, c = t // CORES, t % CORES

    def at(zz, yy, xx, cc):
        return (zz * ny + yy, xx * CORES + cc)

    return z, y, x, c, at


def greet(devices):
    barrier = pltpu.get_barrier_semaphore()
    for device in devices:
        pl.semaphore_signal(barrier, inc=1, device_id=device, device_id_type=MESH)
    pl.semaphore_wait(barrier, len(devices))


def spread_kernel(
    ny, nz, nx, lat_ref, up_ref, dn_ref, lat_out, up_out, dn_out,
    own_sem, lz_s, lz_r, ly_s, ly_r, lc_s, lc_r, uz_s, uz_r, uy_s, uy_r, dz_s, dz_r, dy_s, dy_r,
):
    z, y, x, c, at = place(ny, nz, nx)
    s = z * ny + y
    rows = lat_ref.shape[0]
    half = rows // CORES
    units = up_out.shape[2]
    mine = pl.ds(pl.multiple_of(c * half, half), half)
    other = pl.ds(pl.multiple_of((1 - c) * half, half), half)
    partner = at(z, y, x, 1 - c)
    zdev = [at((z + k) % nz, y, x, c) for k in range(nz)]
    ydev = [at(z, (y + j) % ny, x, c) for j in range(ny)]
    greet(zdev[1:] + ydev[1:] + [partner])

    def block(k, j):
        return ((z - k + nz) % nz) * ny + (y - j + ny) % ny

    def up_part(to):
        return up_ref.at[:, pl.ds(pl.multiple_of(to * units, LANES), units)]

    def dn_part(to):
        return dn_ref.at[pl.ds(pl.multiple_of(to * units, LANES), units), :]

    sent = []

    def start(*args):
        copy = remote(*args)
        copy.start()
        sent.append(copy)

    for k in range(1, nz):
        start(lat_ref.at[mine], lat_out.at[s, mine], lz_s.at[k], lz_r.at[k], zdev[k])
    for j in range(1, ny):
        start(lat_ref.at[mine], lat_out.at[s, mine], ly_s.at[0, j], ly_r.at[0, j], ydev[j])
    for k in range(1, nz):
        to = (z + k) % nz
        start(up_part(to), up_out.at[s], uz_s.at[k], uz_r.at[k], zdev[k])
        start(dn_part(to), dn_out.at[s], dz_s.at[k], dz_r.at[k], zdev[k])
    own = [
        pltpu.make_async_copy(lat_ref, lat_out.at[s], own_sem.at[0]),
        pltpu.make_async_copy(up_part(z), up_out.at[s], own_sem.at[1]),
        pltpu.make_async_copy(dn_part(z), dn_out.at[s], own_sem.at[2]),
    ]
    for copy in own:
        copy.start()

    def to_partner(k, j):
        slot = lat_out.at[block(k, j), mine]
        start(slot, slot, lc_s.at[k, j], lc_r.at[k, j], partner)

    for k in range(1, nz):
        slot = lat_out.at[block(k, 0), mine]
        remote(slot, slot, lz_s.at[k], lz_r.at[k], zdev[k]).wait_recv()
        for j in range(1, ny):
            start(slot, slot, ly_s.at[k, j], ly_r.at[k, j], ydev[j])
        to_partner(k, 0)
    for j in range(1, ny):
        start(up_part(z), up_out.at[s], uy_s.at[0, j], uy_r.at[0, j], ydev[j])
        start(dn_part(z), dn_out.at[s], dy_s.at[0, j], dy_r.at[0, j], ydev[j])
    for k in range(nz):
        for j in range(1, ny):
            slot = lat_out.at[block(k, j), mine]
            remote(slot, slot, ly_s.at[k, j], ly_r.at[k, j], ydev[j]).wait_recv()
            to_partner(k, j)
    for k in range(nz):
        for j in range(ny):
            if k or j:
                slot = lat_out.at[block(k, j), other]
                remote(slot, slot, lc_s.at[k, j], lc_r.at[k, j], partner).wait_recv()
    for copy in own:
        copy.wait()
    for k in range(1, nz):
        for out, ss, rs, sy, ry in (
            (up_out, uz_s, uz_r, uy_s, uy_r),
            (dn_out, dz_s, dz_r, dy_s, dy_r),
        ):
            slot = out.at[block(k, 0)]
            remote(slot, slot, ss.at[k], rs.at[k], zdev[k]).wait_recv()
            for j in range(1, ny):
                start(slot, slot, sy.at[k, j], ry.at[k, j], ydev[j])
    for k in range(nz):
        for j in range(1, ny):
            for out, sy, ry in ((up_out, uy_s, uy_r), (dn_out, dy_s, dy_r)):
                slot = out.at[block(k, j)]
                remote(slot, slot, sy.at[k, j], ry.at[k, j], ydev[j]).wait_recv()
    for copy in sent:
        copy.wait_send()


def spread(ny, nz, nx, latents, w_up, w_down):
    rows, width = latents.shape
    units = w_up.shape[1] // nz
    sp = ny * nz
    dma = pltpu.SemaphoreType.DMA
    vmem = pl.BlockSpec(memory_space=pltpu.VMEM)
    return pl.pallas_call(
        functools.partial(spread_kernel, ny, nz, nx),
        out_shape=(
            jax.ShapeDtypeStruct((sp, rows, width), latents.dtype),
            jax.ShapeDtypeStruct((sp, w_up.shape[0], units), w_up.dtype),
            jax.ShapeDtypeStruct((sp, units, w_down.shape[1]), w_down.dtype),
        ),
        in_specs=[vmem] * 3,
        out_specs=(vmem,) * 3,
        scratch_shapes=[dma((3,)), dma((nz,)), dma((nz,))]
        + [dma((nz, ny))] * 4
        + [dma((nz,)), dma((nz,)), dma((nz, ny)), dma((nz, ny))] * 2,
        compiler_params=pltpu.CompilerParams(
            collective_id=1, has_side_effects=True, vmem_limit_bytes=60 * 2**20
        ),
        name="spread",
    )(latents, w_up, w_down)


def mixer_kernel(
    ny, nz, nx, part_ref, resid_ref, gain_ref, up_ref, dn_ref, out_ref,
    rs_in, after, xg, pbuf, cbuf, xbuf, zsend, zbuf,
    a_s, a_r, bz_s, bz_r, bx_s, bx_r, bc_s, bc_r, cc_s, cc_r, cx_s, cx_r, cz_s, cz_r,
):
    z, y, x, c, at = place(ny, nz, nx)
    tp = nx * CORES
    t = x * CORES + c
    rows, width = resid_ref.shape
    partner = at(z, y, x, 1 - c)
    zdev = [at((z + k) % nz, y, x, c) for k in range(nz)]
    zback = [at((z - k + nz) % nz, y, x, c) for k in range(nz)]
    xdev = [at(z, y, (x + j) % nx, c) for j in range(nx)]
    tdev = [(z * ny + y, (t + k) % tp) for k in range(tp)]
    greet(tdev[1:] + zdev[1:])
    sent = []

    def start(*args):
        copy = remote(*args)
        copy.start()
        sent.append(copy)

    for k in range(1, tp):
        start(part_ref.at[(t + k) % tp], rs_in.at[k], a_s.at[k], a_r.at[k], tdev[k])
    total = resid_ref[...].astype(jnp.float32)
    mixed = part_ref[t].astype(jnp.float32)
    for k in range(1, tp):
        remote(rs_in.at[k], rs_in.at[k], a_s.at[k], a_r.at[k], tdev[k]).wait_recv()
        mixed = mixed + rs_in[k].astype(jnp.float32)
    total = (total + mixed).astype(jnp.bfloat16)
    after[...] = total
    xg[z, c, x] = rms_scale(total, gain_ref[...]).astype(jnp.bfloat16)

    def zi(k):
        return (z - k + nz) % nz

    def xi(j):
        return (x - j + nx) % nx

    def gather_step(k):
        slot = xg.at[zi(k), c, x]
        if k == 0:
            for kk in range(1, nz):
                start(slot, slot, bz_s.at[kk], bz_r.at[kk], zdev[kk])
        else:
            remote(slot, slot, bz_s.at[k], bz_r.at[k], zdev[k]).wait_recv()
        for j in range(1, nx):
            start(slot, slot, bx_s.at[k, j], bx_r.at[k, j], xdev[j])
        start(slot, slot, bc_s.at[k, 0], bc_r.at[k, 0], partner)

    def cross_step(k):
        for j in range(1, nx):
            slot = xg.at[zi(k), c, xi(j)]
            remote(slot, slot, bx_s.at[k, j], bx_r.at[k, j], xdev[j]).wait_recv()
            start(slot, slot, bc_s.at[k, j], bc_r.at[k, j], partner)
        for j in range(nx):
            slot = xg.at[zi(k), 1 - c, xi(j)]
            remote(slot, slot, bc_s.at[k, j], bc_r.at[k, j], partner).wait_recv()

    def compute_step(k):
        tokens = xg[zi(k)].reshape(tp * rows, width)
        projected = jnp.dot(tokens, up_ref[...], preferred_element_type=jnp.float32)
        hidden = jnp.square(jnp.maximum(projected, 0.0)).astype(jnp.bfloat16)
        cols = dn_ref.shape[2]
        for b in range(dn_ref.shape[0]):
            block = jnp.dot(hidden, dn_ref[b], preferred_element_type=jnp.float32)
            pbuf[k, :, :, :, b * cols : (b + 1) * cols] = block.astype(jnp.bfloat16).reshape(
                CORES, nx, rows, cols
            )
        start(pbuf.at[k, 1 - c], cbuf.at[k], cc_s.at[k], cc_r.at[k], partner)

    def core_sum(k):
        remote(cbuf.at[k], cbuf.at[k], cc_s.at[k], cc_r.at[k], partner).wait_recv()
        pbuf[k, c] = (
            pbuf[k, c].astype(jnp.float32) + cbuf[k].astype(jnp.float32)
        ).astype(jnp.bfloat16)
        for j in range(1, nx):
            start(pbuf.at[k, c, (x + j) % nx], xbuf.at[k, j], cx_s.at[k, j], cx_r.at[k, j], xdev[j])

    def cross_sum(k):
        summed = pbuf[k, c, x].astype(jnp.float32)
        for j in range(1, nx):
            remote(xbuf.at[k, j], xbuf.at[k, j], cx_s.at[k, j], cx_r.at[k, j], xdev[j]).wait_recv()
            summed = summed + xbuf[k, j].astype(jnp.float32)
        zsend[k] = summed.astype(jnp.bfloat16)
        if k:
            start(zsend.at[k], zbuf.at[k], cz_s.at[k], cz_r.at[k], zback[k])

    gather_step(0)
    for k in range(nz):
        if k + 1 < nz:
            gather_step(k + 1)
        cross_step(k)
        compute_step(k)
        if k >= 1:
            core_sum(k - 1)
        if k >= 2:
            cross_sum(k - 2)
    core_sum(nz - 1)
    for k in range(max(nz - 2, 0), nz):
        cross_sum(k)
    final = after[...].astype(jnp.float32)
    ffn = zsend[0].astype(jnp.float32)
    for k in range(1, nz):
        remote(zbuf.at[k], zbuf.at[k], cz_s.at[k], cz_r.at[k], zback[k]).wait_recv()
        ffn = ffn + zbuf[k].astype(jnp.float32)
    out_ref[...] = (final + ffn).astype(jnp.bfloat16)
    for copy in sent:
        copy.wait_send()


def mixer(ny, nz, nx, part, resid, gain, up, dn):
    tp, rows, width = part.shape
    dma = pltpu.SemaphoreType.DMA
    vmem = pl.BlockSpec(memory_space=pltpu.VMEM)
    b16 = jnp.bfloat16

    def pair(*shape):
        return [dma(shape), dma(shape)]

    return pl.pallas_call(
        functools.partial(mixer_kernel, ny, nz, nx),
        out_shape=jax.ShapeDtypeStruct((rows, width), b16),
        in_specs=[vmem] * 5,
        out_specs=vmem,
        scratch_shapes=[
            pltpu.VMEM((tp, rows, width), b16),
            pltpu.VMEM((rows, width), b16),
            pltpu.VMEM((nz, CORES, nx, rows, width), b16),
            pltpu.VMEM((nz, CORES, nx, rows, width), b16),
            pltpu.VMEM((nz, nx, rows, width), b16),
            pltpu.VMEM((nz, nx, rows, width), b16),
            pltpu.VMEM((nz, rows, width), b16),
            pltpu.VMEM((nz, rows, width), b16),
        ]
        + pair(tp)
        + pair(nz)
        + pair(nz, nx)
        + pair(nz, nx)
        + pair(nz)
        + pair(nz, nx)
        + pair(nz),
        compiler_params=pltpu.CompilerParams(
            collective_id=2, has_side_effects=True, vmem_limit_bytes=60 * 2**20
        ),
        name="mixer",
    )(part, resid, gain, up, dn)


def on_device(
    ny,
    nz,
    nx,
    resid,
    q_latent,
    kv_latent,
    rope_key,
    q_gain,
    kv_gain,
    w_q_small,
    w_q_large,
    w_kv_small,
    w_kv_large,
    w_out_small,
    w_out_large,
    ffn_gain,
    w_up,
    w_down,
):
    tok_rows = q_latent.shape[0]
    offset = lax.axis_index("sp") * tok_rows
    positions = offset + jnp.arange(tok_rows, dtype=jnp.int32)
    last_query = offset + tok_rows - 1
    query_normed = rms_scale(q_latent, q_gain).astype(jnp.bfloat16)
    query_small = queries(query_normed, w_q_small, SMALL_DIM, positions)
    query_large = queries(query_normed, w_q_large, LARGE_DIM, positions)
    key_normed = rms_scale(kv_latent, kv_gain).astype(jnp.bfloat16)
    key_rotated = rotary(rope_key.astype(jnp.float32), positions).astype(jnp.bfloat16)
    small_heads = query_small.shape[1]
    large_heads = query_large.shape[1]

    def empty_state(head_count, head_width):
        return (
            jnp.full((head_count, tok_rows), mask_floor, jnp.float32),
            jnp.zeros((head_count, tok_rows), jnp.float32),
            jnp.zeros((head_count, tok_rows, head_width), jnp.float32),
        )

    initial = (empty_state(small_heads, SMALL_DIM), empty_state(large_heads, LARGE_DIM))

    def from_latent(block_parts):
        latent_block, rot_block = block_parts
        small_kv = jnp.dot(latent_block, w_kv_small, preferred_element_type=jnp.float32).astype(
            jnp.bfloat16
        )
        large_kv = jnp.dot(latent_block, w_kv_large, preferred_element_type=jnp.float32).astype(
            jnp.bfloat16
        )
        return (small_kv, large_kv, rot_block)

    folded = initial
    rope_pad = jnp.pad(key_rotated, ((0, 0), (0, LANES - ROPE_DIM)))
    latents, up_mine, down_mine = spread(
        ny, nz, nx, jnp.concatenate([key_normed, rope_pad], axis=1), w_up, w_down
    )
    latents = latents.reshape(-1, latents.shape[-1])
    rank = key_normed.shape[1]
    pieces = (latents[:, :rank], latents[:, rank : rank + ROPE_DIM])
    piece_rows = pieces[0].shape[0]
    block_rows = math.gcd(piece_rows, 512)
    block_count = piece_rows // block_rows
    blocked = tuple((p.reshape(block_count, block_rows, p.shape[1]) for p in pieces))

    def key_step(running, block_args):
        block_parts, block_index = block_args
        key_pos = block_index * block_rows + jnp.arange(block_rows, dtype=jnp.int32)

        def attend(state):
            small_kv, large_kv, rot_block = from_latent(block_parts)
            small_kv = small_kv.reshape(block_rows, small_heads, 2 * SMALL_DIM)
            large_kv = large_kv.reshape(block_rows, large_heads, 2 * LARGE_DIM)
            small_state = update_group(
                state[0],
                query_small,
                small_kv[..., :SMALL_DIM],
                small_kv[..., SMALL_DIM:],
                rot_block,
                positions,
                key_pos,
                SMALL_DIM,
            )
            large_state = update_group(
                state[1],
                query_large,
                large_kv[..., :LARGE_DIM],
                large_kv[..., LARGE_DIM:],
                rot_block,
                positions,
                key_pos,
                LARGE_DIM,
            )
            return (small_state, large_state)

        def unchanged(state):
            return state

        running = lax.cond(key_pos[0] <= last_query, attend, unchanged, running)
        return (running, None)

    folded, unused = lax.scan(key_step, folded, (blocked, jnp.arange(block_count, dtype=jnp.int32)))

    def finish(running):
        row_max, row_sum, weighted = running
        normalized = weighted / row_sum[..., None]
        return jnp.transpose(normalized, (1, 0, 2)).reshape(tok_rows, -1).astype(jnp.bfloat16)

    attn_small = finish(folded[0])
    attn_large = finish(folded[1])
    part = (
        jnp.dot(attn_small, w_out_small, preferred_element_type=jnp.float32)
        + jnp.dot(attn_large, w_out_large, preferred_element_type=jnp.float32)
    ).astype(jnp.bfloat16)
    width = part.shape[1]
    return mixer(
        ny,
        nz,
        nx,
        part.reshape(nx * CORES, -1, width),
        resid,
        ffn_gain.reshape(1, width),
        up_mine.reshape(width, -1),
        down_mine,
    )


def solution(mesh):
    ny = inner_split(mesh.shape["sp"])
    nz = mesh.shape["sp"] // ny
    nx = mesh.shape["tp"] // CORES
    return jax.shard_map(
        functools.partial(on_device, ny, nz, nx),
        mesh=mesh,
        in_specs=(
            P(("sp", "tp"), None),
            P("sp", None),
            P("sp", None),
            P("sp", None),
            P(),
            P(),
            P(None, "tp"),
            P(None, "tp"),
            P(None, "tp"),
            P(None, "tp"),
            P("tp", None),
            P("tp", None),
            P(),
            P("sp", "tp"),
            P("tp", "sp"),
        ),
        out_specs=P(("sp", "tp"), None),
        check_vma=False,
    )
```

```python
import functools

import jax
import jax.numpy as jnp
from jax import lax
from jax.experimental import pallas as pl
from jax.experimental.pallas import tpu as pltpu
from jax.sharding import PartitionSpec as P

SMALL_DIM = 64
LARGE_DIM = 128
ROPE_DIM = 32


epsilon = 1e-06
theta_base = 10000.0
mask_floor = -1e30


def rms_scale(inputs, gain_vec):
    values = inputs.astype(jnp.float32)
    return (
        values * lax.rsqrt(jnp.mean(values * values, axis=-1, keepdims=True) + epsilon) * gain_vec
    )


def rotary(values, positions):
    halfway = values.shape[-1] // 2
    inverse = theta_base ** (-jnp.arange(0, 2 * halfway, 2, dtype=jnp.float32) / (2 * halfway))
    angles = positions.astype(jnp.float32)[:, None] * inverse[None, :]
    cos_table = jnp.cos(angles)
    sin_table = jnp.sin(angles)
    if values.ndim == 3:
        cos_table = cos_table[:, None, :]
        sin_table = sin_table[:, None, :]
    first_half = values[..., :halfway]
    second_half = values[..., halfway:]
    return jnp.concatenate(
        [
            first_half * cos_table - second_half * sin_table,
            second_half * cos_table + first_half * sin_table,
        ],
        axis=-1,
    )


def queries(normed, weight, nope_dim, positions):
    projected = jnp.dot(normed, weight, preferred_element_type=jnp.float32)
    projected = projected.reshape(projected.shape[0], -1, nope_dim + ROPE_DIM)
    turned = rotary(projected[..., nope_dim:], positions)
    return jnp.concatenate([projected[..., :nope_dim], turned], axis=-1).astype(jnp.bfloat16)


MESH = pl.DeviceIdType.MESH
CORES = 2
LANES = 128


def inner_split(count):
    best = 1
    for size in range(1, count + 1):
        if size * size <= count and count % size == 0:
            best = size
    return best


def remote(src, dst, send_sem, recv_sem, device):
    return pltpu.make_async_remote_copy(
        src_ref=src,
        dst_ref=dst,
        send_sem=send_sem,
        recv_sem=recv_sem,
        device_id=device,
        device_id_type=MESH,
    )


def place(ny, nz, nx):
    s, t = lax.axis_index("sp"), lax.axis_index("tp")
    z, y = s // ny, s % ny
    x, c = t // CORES, t % CORES

    def at(zz, yy, xx, cc):
        return (zz * ny + yy, xx * CORES + cc)

    return z, y, x, c, at


def greet(devices):
    barrier = pltpu.get_barrier_semaphore()
    for device in devices:
        pl.semaphore_signal(barrier, inc=1, device_id=device, device_id_type=MESH)
    pl.semaphore_wait(barrier, len(devices))


def layer_kernel(
    ny, nz, nx, lat_ref, q_ref, wks_ref, wkl_ref, wos_ref, wol_ref, resid_ref, gain_ref, up_ref,
    dn_ref, out_ref, lat_out, up_out, dn_out, row_max, row_sum, weighted, part_ref,
    rs_in, after, xg, pbuf, cbuf, xbuf, zsend, zbuf, own_sem,
    lz_s, lz_r, ly_s, ly_r, lc_s, lc_r, uz_s, uz_r, uy_s, uy_r, dz_s, dz_r, dy_s, dy_r,
    a_s, a_r, bz_s, bz_r, bx_s, bx_r, bc_s, bc_r, cc_s, cc_r, cx_s, cx_r, cz_s, cz_r,
):
    z, y, x, c, at = place(ny, nz, nx)
    s = z * ny + y
    rows = lat_ref.shape[0]
    half = rows // CORES
    units = up_out.shape[2]
    tp = nx * CORES
    t = x * CORES + c
    mine = pl.ds(pl.multiple_of(c * half, half), half)
    other = pl.ds(pl.multiple_of((1 - c) * half, half), half)
    partner = at(z, y, x, 1 - c)
    zdev = [at((z + k) % nz, y, x, c) for k in range(nz)]
    ydev = [at(z, (y + j) % ny, x, c) for j in range(ny)]
    zback = [at((z - k + nz) % nz, y, x, c) for k in range(nz)]
    xdev = [at(z, y, (x + j) % nx, c) for j in range(nx)]
    tdev = [(s, (t + k) % tp) for k in range(tp)]
    greet(zdev[1:] + ydev[1:] + tdev[1:])

    def block(k, j):
        return ((z - k + nz) % nz) * ny + (y - j + ny) % ny

    def up_part(to):
        return up_ref.at[:, pl.ds(pl.multiple_of(to * units, LANES), units)]

    def dn_part(to):
        return dn_ref.at[pl.ds(pl.multiple_of(to * units, LANES), units), :]

    sent = []

    def start(*args):
        copy = remote(*args)
        copy.start()
        sent.append(copy)

    for k in range(1, nz):
        start(lat_ref.at[mine], lat_out.at[s, mine], lz_s.at[k], lz_r.at[k], zdev[k])
    for j in range(1, ny):
        start(lat_ref.at[mine], lat_out.at[s, mine], ly_s.at[0, j], ly_r.at[0, j], ydev[j])
    for k in range(1, nz):
        to = (z + k) % nz
        start(up_part(to), up_out.at[s], uz_s.at[k], uz_r.at[k], zdev[k])
        start(dn_part(to), dn_out.at[s], dz_s.at[k], dz_r.at[k], zdev[k])
    own = [
        pltpu.make_async_copy(lat_ref, lat_out.at[s], own_sem.at[0]),
        pltpu.make_async_copy(up_part(z), up_out.at[s], own_sem.at[1]),
        pltpu.make_async_copy(dn_part(z), dn_out.at[s], own_sem.at[2]),
    ]
    for copy in own:
        copy.start()

    def to_partner(k, j):
        slot = lat_out.at[block(k, j), mine]
        start(slot, slot, lc_s.at[k, j], lc_r.at[k, j], partner)

    for k in range(1, nz):
        slot = lat_out.at[block(k, 0), mine]
        remote(slot, slot, lz_s.at[k], lz_r.at[k], zdev[k]).wait_recv()
        for j in range(1, ny):
            start(slot, slot, ly_s.at[k, j], ly_r.at[k, j], ydev[j])
        to_partner(k, 0)
    for j in range(1, ny):
        start(up_part(z), up_out.at[s], uy_s.at[0, j], uy_r.at[0, j], ydev[j])
        start(dn_part(z), dn_out.at[s], dy_s.at[0, j], dy_r.at[0, j], ydev[j])
    for k in range(nz):
        for j in range(1, ny):
            slot = lat_out.at[block(k, j), mine]
            remote(slot, slot, ly_s.at[k, j], ly_r.at[k, j], ydev[j]).wait_recv()
            to_partner(k, j)
    for k in range(nz):
        for j in range(ny):
            if k or j:
                slot = lat_out.at[block(k, j), other]
                remote(slot, slot, lc_s.at[k, j], lc_r.at[k, j], partner).wait_recv()
    for copy in own:
        copy.wait()

    def forward(k):
        for out, ss, rs, sy, ry in (
            (up_out, uz_s, uz_r, uy_s, uy_r),
            (dn_out, dz_s, dz_r, dy_s, dy_r),
        ):
            slot = out.at[block(k, 0)]
            remote(slot, slot, ss.at[k], rs.at[k], zdev[k]).wait_recv()
            for j in range(1, ny):
                start(slot, slot, sy.at[k, j], ry.at[k, j], ydev[j])

    rank = wks_ref.shape[0]
    heads = q_ref.shape[0]
    small = wks_ref.shape[1] // (2 * SMALL_DIM)
    row_max[...] = jnp.full_like(row_max, mask_floor)
    row_sum[...] = jnp.zeros_like(row_sum)
    weighted[...] = jnp.zeros_like(weighted)
    ahead = lax.broadcasted_iota(jnp.int32, (rows, rows), 1) - lax.broadcasted_iota(
        jnp.int32, (rows, rows), 0
    )

    def key_step(j, carry):
        latent = lat_out[j, :, :rank]
        turned = lat_out[j, :, rank:]
        kv_small = jnp.dot(latent, wks_ref[...], preferred_element_type=jnp.float32)
        kv_small = kv_small.astype(jnp.bfloat16)
        kv_large = jnp.dot(latent, wkl_ref[...], preferred_element_type=jnp.float32)
        kv_large = kv_large.astype(jnp.bfloat16)
        causal = ahead <= (s - j) * rows
        for h in range(heads):
            if h < small:
                key = kv_small[:, 2 * SMALL_DIM * h : 2 * SMALL_DIM * (h + 1)]
                value = key
                scale = (SMALL_DIM + ROPE_DIM) ** (-0.5)
            else:
                first = 2 * LARGE_DIM * (h - small)
                key = kv_large[:, first : first + LARGE_DIM]
                value = kv_large[:, first + LARGE_DIM : first + 2 * LARGE_DIM]
                scale = (LARGE_DIM + ROPE_DIM) ** (-0.5)
            scores = lax.dot_general(
                q_ref[h],
                jnp.concatenate([key, turned], axis=1),
                (((1,), (1,)), ((), ())),
                preferred_element_type=jnp.float32,
            )
            scores = jnp.where(causal, scores * scale, mask_floor)
            old_max = row_max[h]
            new_max = jnp.maximum(old_max, jnp.max(scores, axis=-1, keepdims=True))
            shrink = jnp.exp(old_max - new_max)
            weights = jnp.exp(scores - new_max)
            row_max[h] = new_max
            row_sum[h] = row_sum[h] * shrink + jnp.sum(weights, axis=-1, keepdims=True)
            weighted[h] = weighted[h] * shrink + jnp.dot(
                weights.astype(jnp.bfloat16), value, preferred_element_type=jnp.float32
            )
        return carry

    middle = (s + 1) // 2
    lax.fori_loop(0, middle, key_step, 0)
    if nz > 1:
        forward(1)
    lax.fori_loop(middle, s + 1, key_step, 0)
    for k in range(2, nz - 1):
        forward(k)
    parts = []
    for h in range(heads):
        head_out = (weighted[h] / row_sum[h]).astype(jnp.bfloat16)
        parts.append(head_out[:, SMALL_DIM:] if h < small else head_out)
    mixed_part = jnp.dot(
        jnp.concatenate(parts[:small], axis=1), wos_ref[...], preferred_element_type=jnp.float32
    ) + jnp.dot(
        jnp.concatenate(parts[small:], axis=1), wol_ref[...], preferred_element_type=jnp.float32
    )
    part_ref[...] = mixed_part.astype(jnp.bfloat16).reshape(part_ref.shape)
    rows, width = resid_ref.shape
    for k in range(1, tp):
        start(part_ref.at[(t + k) % tp], rs_in.at[k], a_s.at[k], a_r.at[k], tdev[k])
    if nz > 2:
        forward(nz - 1)
    total = resid_ref[...].astype(jnp.float32)
    mixed = part_ref[t].astype(jnp.float32)
    for k in range(1, tp):
        remote(rs_in.at[k], rs_in.at[k], a_s.at[k], a_r.at[k], tdev[k]).wait_recv()
        mixed = mixed + rs_in[k].astype(jnp.float32)
    total = (total + mixed).astype(jnp.bfloat16)
    after[...] = total
    xg[z, c, x] = rms_scale(total, gain_ref[...]).astype(jnp.bfloat16)

    def zi(k):
        return (z - k + nz) % nz

    def xi(j):
        return (x - j + nx) % nx

    def gather_step(k):
        slot = xg.at[zi(k), c, x]
        if k == 0:
            for kk in range(1, nz):
                start(slot, slot, bz_s.at[kk], bz_r.at[kk], zdev[kk])
        else:
            remote(slot, slot, bz_s.at[k], bz_r.at[k], zdev[k]).wait_recv()
        for j in range(1, nx):
            start(slot, slot, bx_s.at[k, j], bx_r.at[k, j], xdev[j])
        start(slot, slot, bc_s.at[k, 0], bc_r.at[k, 0], partner)

    def cross_step(k):
        for j in range(1, nx):
            slot = xg.at[zi(k), c, xi(j)]
            remote(slot, slot, bx_s.at[k, j], bx_r.at[k, j], xdev[j]).wait_recv()
            start(slot, slot, bc_s.at[k, j], bc_r.at[k, j], partner)
        for j in range(nx):
            slot = xg.at[zi(k), 1 - c, xi(j)]
            remote(slot, slot, bc_s.at[k, j], bc_r.at[k, j], partner).wait_recv()

    def compute_step(k):
        tokens = xg[zi(k)].reshape(tp * rows, width)
        projected = jnp.dot(tokens, up_out[...].reshape(width, units), preferred_element_type=jnp.float32)
        hidden = jnp.square(jnp.maximum(projected, 0.0)).astype(jnp.bfloat16)
        cols = dn_out.shape[2]
        for b in range(dn_out.shape[0]):
            block = jnp.dot(hidden, dn_out[b], preferred_element_type=jnp.float32)
            pbuf[k, :, :, :, b * cols : (b + 1) * cols] = block.astype(jnp.bfloat16).reshape(
                CORES, nx, rows, cols
            )
        start(pbuf.at[k, 1 - c], cbuf.at[k], cc_s.at[k], cc_r.at[k], partner)

    def core_sum(k):
        remote(cbuf.at[k], cbuf.at[k], cc_s.at[k], cc_r.at[k], partner).wait_recv()
        pbuf[k, c] = (
            pbuf[k, c].astype(jnp.float32) + cbuf[k].astype(jnp.float32)
        ).astype(jnp.bfloat16)
        for j in range(1, nx):
            start(pbuf.at[k, c, (x + j) % nx], xbuf.at[k, j], cx_s.at[k, j], cx_r.at[k, j], xdev[j])

    def cross_sum(k):
        summed = pbuf[k, c, x].astype(jnp.float32)
        for j in range(1, nx):
            remote(xbuf.at[k, j], xbuf.at[k, j], cx_s.at[k, j], cx_r.at[k, j], xdev[j]).wait_recv()
            summed = summed + xbuf[k, j].astype(jnp.float32)
        zsend[k] = summed.astype(jnp.bfloat16)
        if k:
            start(zsend.at[k], zbuf.at[k], cz_s.at[k], cz_r.at[k], zback[k])

    def weights_here():
        for k in range(nz):
            for j in range(1, ny):
                for out, sy, ry in ((up_out, uy_s, uy_r), (dn_out, dy_s, dy_r)):
                    slot = out.at[block(k, j)]
                    remote(slot, slot, sy.at[k, j], ry.at[k, j], ydev[j]).wait_recv()

    gather_step(0)
    for k in range(nz):
        if k + 1 < nz:
            gather_step(k + 1)
        cross_step(k)
        if k == 0:
            weights_here()
        compute_step(k)
        if k >= 1:
            core_sum(k - 1)
        if k >= 2:
            cross_sum(k - 2)
    core_sum(nz - 1)
    for k in range(max(nz - 2, 0), nz):
        cross_sum(k)
    final = after[...].astype(jnp.float32)
    ffn = zsend[0].astype(jnp.float32)
    for k in range(1, nz):
        remote(zbuf.at[k], zbuf.at[k], cz_s.at[k], cz_r.at[k], zback[k]).wait_recv()
        ffn = ffn + zbuf[k].astype(jnp.float32)
    out_ref[...] = (final + ffn).astype(jnp.bfloat16)
    for copy in sent:
        copy.wait_send()


def layer(ny, nz, nx, latents, q_all, wks, wkl, wos, wol, resid, gain, w_up, w_down):
    tp, sp = nx * CORES, ny * nz
    rows, width = resid.shape
    tok_rows = latents.shape[0]
    heads = q_all.shape[0]
    units = w_up.shape[1] // nz
    dma = pltpu.SemaphoreType.DMA
    vmem = pl.BlockSpec(memory_space=pltpu.VMEM)
    b16 = jnp.bfloat16

    def pair(*shape):
        return [dma(shape), dma(shape)]

    return pl.pallas_call(
        functools.partial(layer_kernel, ny, nz, nx),
        out_shape=jax.ShapeDtypeStruct((rows, width), b16),
        in_specs=[vmem] * 10,
        out_specs=vmem,
        scratch_shapes=[
            pltpu.VMEM((sp,) + latents.shape, b16),
            pltpu.VMEM((sp, w_up.shape[0], units), b16),
            pltpu.VMEM((sp, units, w_down.shape[1]), b16),
            pltpu.VMEM((heads, tok_rows, 1), jnp.float32),
            pltpu.VMEM((heads, tok_rows, 1), jnp.float32),
            pltpu.VMEM((heads, tok_rows, LARGE_DIM), jnp.float32),
            pltpu.VMEM((tp, rows, width), b16),
            pltpu.VMEM((tp, rows, width), b16),
            pltpu.VMEM((rows, width), b16),
            pltpu.VMEM((nz, CORES, nx, rows, width), b16),
            pltpu.VMEM((nz, CORES, nx, rows, width), b16),
            pltpu.VMEM((nz, nx, rows, width), b16),
            pltpu.VMEM((nz, nx, rows, width), b16),
            pltpu.VMEM((nz, rows, width), b16),
            pltpu.VMEM((nz, rows, width), b16),
            dma((3,)),
        ]
        + pair(nz)
        + pair(nz, ny) * 2
        + (pair(nz) + pair(nz, ny)) * 2
        + pair(tp)
        + pair(nz)
        + pair(nz, nx)
        + pair(nz, nx)
        + pair(nz)
        + pair(nz, nx)
        + pair(nz),
        compiler_params=pltpu.CompilerParams(
            collective_id=1, has_side_effects=True, vmem_limit_bytes=63 * 2**20
        ),
        name="layer",
    )(latents, q_all, wks, wkl, wos, wol, resid, gain, w_up, w_down)


def on_device(
    ny,
    nz,
    nx,
    resid,
    q_latent,
    kv_latent,
    rope_key,
    q_gain,
    kv_gain,
    w_q_small,
    w_q_large,
    w_kv_small,
    w_kv_large,
    w_out_small,
    w_out_large,
    ffn_gain,
    w_up,
    w_down,
):
    tok_rows = q_latent.shape[0]
    offset = lax.axis_index("sp") * tok_rows
    positions = offset + jnp.arange(tok_rows, dtype=jnp.int32)
    query_normed = rms_scale(q_latent, q_gain).astype(jnp.bfloat16)
    query_small = queries(query_normed, w_q_small, SMALL_DIM, positions)
    query_large = queries(query_normed, w_q_large, LARGE_DIM, positions)
    key_normed = rms_scale(kv_latent, kv_gain).astype(jnp.bfloat16)
    key_rotated = rotary(rope_key.astype(jnp.float32), positions).astype(jnp.bfloat16)
    rope_pad = ((0, 0), (0, LANES - ROPE_DIM))
    latents = jnp.concatenate([key_normed, jnp.pad(key_rotated, rope_pad)], axis=1)

    def head_rows(query, nope_dim):
        content = jnp.pad(query[..., :nope_dim], ((0, 0), (0, 0), (0, LARGE_DIM - nope_dim)))
        turned = jnp.pad(query[..., nope_dim:], ((0, 0),) + rope_pad)
        return jnp.transpose(jnp.concatenate([content, turned], axis=-1), (1, 0, 2))

    q_all = jnp.concatenate(
        [head_rows(query_small, SMALL_DIM), head_rows(query_large, LARGE_DIM)], axis=0
    )
    return layer(
        ny,
        nz,
        nx,
        latents,
        q_all,
        w_kv_small,
        w_kv_large,
        w_out_small,
        w_out_large,
        resid,
        ffn_gain.reshape(1, -1),
        w_up,
        w_down,
    )


def solution(mesh):
    ny = inner_split(mesh.shape["sp"])
    nz = mesh.shape["sp"] // ny
    nx = mesh.shape["tp"] // CORES
    return jax.shard_map(
        functools.partial(on_device, ny, nz, nx),
        mesh=mesh,
        in_specs=(
            P(("sp", "tp"), None),
            P("sp", None),
            P("sp", None),
            P("sp", None),
            P(),
            P(),
            P(None, "tp"),
            P(None, "tp"),
            P(None, "tp"),
            P(None, "tp"),
            P("tp", None),
            P("tp", None),
            P(),
            P("sp", "tp"),
            P("tp", "sp"),
        ),
        out_specs=P(("sp", "tp"), None),
        check_vma=False,
    )
```

```python
import functools

import jax
import jax.numpy as jnp
from jax import lax
from jax.experimental import pallas as pl
from jax.experimental.pallas import tpu as pltpu
from jax.sharding import PartitionSpec as P

SMALL_DIM = 64
LARGE_DIM = 128
ROPE_DIM = 32


epsilon = 1e-06
theta_base = 10000.0
mask_floor = -1e30


def rms_scale(inputs, gain_vec):
    values = inputs.astype(jnp.float32)
    return (
        values * lax.rsqrt(jnp.mean(values * values, axis=-1, keepdims=True) + epsilon) * gain_vec
    )


def rotary(values, positions):
    halfway = values.shape[-1] // 2
    inverse = theta_base ** (-jnp.arange(0, 2 * halfway, 2, dtype=jnp.float32) / (2 * halfway))
    angles = positions.astype(jnp.float32)[:, None] * inverse[None, :]
    cos_table = jnp.cos(angles)
    sin_table = jnp.sin(angles)
    if values.ndim == 3:
        cos_table = cos_table[:, None, :]
        sin_table = sin_table[:, None, :]
    first_half = values[..., :halfway]
    second_half = values[..., halfway:]
    return jnp.concatenate(
        [
            first_half * cos_table - second_half * sin_table,
            second_half * cos_table + first_half * sin_table,
        ],
        axis=-1,
    )


def queries(normed, weight, nope_dim, positions):
    projected = jnp.dot(normed, weight, preferred_element_type=jnp.float32)
    projected = projected.reshape(projected.shape[0], -1, nope_dim + ROPE_DIM)
    turned = rotary(projected[..., nope_dim:], positions)
    return jnp.concatenate([projected[..., :nope_dim], turned], axis=-1).astype(jnp.bfloat16)


MESH = pl.DeviceIdType.MESH
CORES = 2
LANES = 128


def inner_split(count):
    best = 1
    for size in range(1, count + 1):
        if size * size <= count and count % size == 0:
            best = size
    return best


def remote(src, dst, send_sem, recv_sem, device):
    return pltpu.make_async_remote_copy(
        src_ref=src,
        dst_ref=dst,
        send_sem=send_sem,
        recv_sem=recv_sem,
        device_id=device,
        device_id_type=MESH,
    )


def place(ny, nz, nx):
    s, t = lax.axis_index("sp"), lax.axis_index("tp")
    z, y = s // ny, s % ny
    x, c = t // CORES, t % CORES

    def at(zz, yy, xx, cc):
        return (zz * ny + yy, xx * CORES + cc)

    return z, y, x, c, at


def greet(devices):
    barrier = pltpu.get_barrier_semaphore()
    for device in devices:
        pl.semaphore_signal(barrier, inc=1, device_id=device, device_id_type=MESH)
    pl.semaphore_wait(barrier, len(devices))


def layer_kernel(
    ny, nz, nx, lat_ref, q_ref, wks_ref, wkl_ref, wos_ref, wol_ref, resid_ref, gain_ref, up_ref,
    dn_ref, out_ref, lat_out, up_out, dn_out, row_max, row_sum, weighted, part_ref,
    rs_in, after, xg, pbuf, cbuf, xbuf, zsend, zbuf, own_sem,
    lz_s, lz_r, ly_s, ly_r, lc_s, lc_r, uz_s, uz_r, uy_s, uy_r, dz_s, dz_r, dy_s, dy_r,
    a_s, a_r, bz_s, bz_r, bx_s, bx_r, bc_s, bc_r, cc_s, cc_r, cx_s, cx_r, cz_s, cz_r,
):
    z, y, x, c, at = place(ny, nz, nx)
    s = z * ny + y
    rows = lat_ref.shape[0]
    half = rows // CORES
    units = up_out.shape[2]
    tp = nx * CORES
    t = x * CORES + c
    mine = pl.ds(pl.multiple_of(c * half, half), half)
    other = pl.ds(pl.multiple_of((1 - c) * half, half), half)
    partner = at(z, y, x, 1 - c)
    zdev = [at((z + k) % nz, y, x, c) for k in range(nz)]
    ydev = [at(z, (y + j) % ny, x, c) for j in range(ny)]
    zback = [at((z - k + nz) % nz, y, x, c) for k in range(nz)]
    xdev = [at(z, y, (x + j) % nx, c) for j in range(nx)]
    tdev = [(s, (t + k) % tp) for k in range(tp)]
    greet(zdev[1:] + ydev[1:] + tdev[1:])

    def block(k, j):
        return ((z - k + nz) % nz) * ny + (y - j + ny) % ny

    def up_part(to):
        return up_ref.at[:, pl.ds(pl.multiple_of(to * units, LANES), units)]

    def dn_part(to):
        return dn_ref.at[pl.ds(pl.multiple_of(to * units, LANES), units), :]

    sent = []

    def start(*args):
        copy = remote(*args)
        copy.start()
        sent.append(copy)

    for k in range(1, nz):
        start(lat_ref.at[mine], lat_out.at[s, mine], lz_s.at[k], lz_r.at[k], zdev[k])
    for j in range(1, ny):
        start(lat_ref.at[mine], lat_out.at[s, mine], ly_s.at[0, j], ly_r.at[0, j], ydev[j])
    for k in range(1, nz):
        to = (z + k) % nz
        start(up_part(to), up_out.at[s], uz_s.at[k], uz_r.at[k], zdev[k])
        start(dn_part(to), dn_out.at[s], dz_s.at[k], dz_r.at[k], zdev[k])
    own = [
        pltpu.make_async_copy(lat_ref, lat_out.at[s], own_sem.at[0]),
        pltpu.make_async_copy(up_part(z), up_out.at[s], own_sem.at[1]),
        pltpu.make_async_copy(dn_part(z), dn_out.at[s], own_sem.at[2]),
    ]
    for copy in own:
        copy.start()

    def to_partner(k, j):
        slot = lat_out.at[block(k, j), mine]
        start(slot, slot, lc_s.at[k, j], lc_r.at[k, j], partner)

    for k in range(1, nz):
        slot = lat_out.at[block(k, 0), mine]
        remote(slot, slot, lz_s.at[k], lz_r.at[k], zdev[k]).wait_recv()
        for j in range(1, ny):
            start(slot, slot, ly_s.at[k, j], ly_r.at[k, j], ydev[j])
        to_partner(k, 0)
    for j in range(1, ny):
        start(up_part(z), up_out.at[s], uy_s.at[0, j], uy_r.at[0, j], ydev[j])
        start(dn_part(z), dn_out.at[s], dy_s.at[0, j], dy_r.at[0, j], ydev[j])
    for k in range(nz):
        for j in range(1, ny):
            slot = lat_out.at[block(k, j), mine]
            remote(slot, slot, ly_s.at[k, j], ly_r.at[k, j], ydev[j]).wait_recv()
            to_partner(k, j)
    for k in range(nz):
        for j in range(ny):
            if k or j:
                slot = lat_out.at[block(k, j), other]
                remote(slot, slot, lc_s.at[k, j], lc_r.at[k, j], partner).wait_recv()
    for copy in own:
        copy.wait()

    def forward(k):
        for out, ss, rs, sy, ry in (
            (up_out, uz_s, uz_r, uy_s, uy_r),
            (dn_out, dz_s, dz_r, dy_s, dy_r),
        ):
            slot = out.at[block(k, 0)]
            remote(slot, slot, ss.at[k], rs.at[k], zdev[k]).wait_recv()
            for j in range(1, ny):
                start(slot, slot, sy.at[k, j], ry.at[k, j], ydev[j])

    rank = wks_ref.shape[0]
    heads = q_ref.shape[0]
    small = wks_ref.shape[1] // (2 * SMALL_DIM)
    row_max[...] = jnp.full_like(row_max, mask_floor)
    row_sum[...] = jnp.zeros_like(row_sum)
    weighted[...] = jnp.zeros_like(weighted)
    ahead = lax.broadcasted_iota(jnp.int32, (rows, rows), 1) - lax.broadcasted_iota(
        jnp.int32, (rows, rows), 0
    )

    def key_step(j, carry):
        latent = lat_out[j, :, :rank]
        turned = lat_out[j, :, rank:]
        kv_small = jnp.dot(latent, wks_ref[...], preferred_element_type=jnp.float32)
        kv_small = kv_small.astype(jnp.bfloat16)
        kv_large = jnp.dot(latent, wkl_ref[...], preferred_element_type=jnp.float32)
        kv_large = kv_large.astype(jnp.bfloat16)
        causal = ahead <= (s - j) * rows
        for h in range(heads):
            if h < small:
                key = kv_small[:, 2 * SMALL_DIM * h : 2 * SMALL_DIM * (h + 1)]
                value = key
                scale = (SMALL_DIM + ROPE_DIM) ** (-0.5)
            else:
                first = 2 * LARGE_DIM * (h - small)
                key = kv_large[:, first : first + LARGE_DIM]
                value = kv_large[:, first + LARGE_DIM : first + 2 * LARGE_DIM]
                scale = (LARGE_DIM + ROPE_DIM) ** (-0.5)
            scores = lax.dot_general(
                q_ref[h],
                jnp.concatenate([key, turned], axis=1),
                (((1,), (1,)), ((), ())),
                preferred_element_type=jnp.float32,
            )
            scores = jnp.where(causal, scores * scale, mask_floor)
            old_max = row_max[h]
            new_max = jnp.maximum(old_max, jnp.max(scores, axis=-1, keepdims=True))
            shrink = jnp.exp(old_max - new_max)
            weights = jnp.exp(scores - new_max)
            row_max[h] = new_max
            row_sum[h] = row_sum[h] * shrink + jnp.sum(weights, axis=-1, keepdims=True)
            weighted[h] = weighted[h] * shrink + jnp.dot(
                weights.astype(jnp.bfloat16), value, preferred_element_type=jnp.float32
            )
        return carry

    middle = (s + 1) // 2
    lax.fori_loop(0, middle, key_step, 0)
    if nz > 1:
        forward(1)
    lax.fori_loop(middle, s + 1, key_step, 0)
    parts = []
    for h in range(heads):
        head_out = (weighted[h] / row_sum[h]).astype(jnp.bfloat16)
        parts.append(head_out[:, SMALL_DIM:] if h < small else head_out)
    mixed_part = jnp.dot(
        jnp.concatenate(parts[:small], axis=1), wos_ref[...], preferred_element_type=jnp.float32
    ) + jnp.dot(
        jnp.concatenate(parts[small:], axis=1), wol_ref[...], preferred_element_type=jnp.float32
    )
    part_ref[...] = mixed_part.astype(jnp.bfloat16).reshape(part_ref.shape)
    rows, width = resid_ref.shape
    for k in range(1, tp):
        start(part_ref.at[(t + k) % tp], rs_in.at[k], a_s.at[k], a_r.at[k], tdev[k])
    for k in range(2, nz - 1):
        forward(k)
    total = resid_ref[...].astype(jnp.float32)
    mixed = part_ref[t].astype(jnp.float32)
    for k in range(1, tp):
        remote(rs_in.at[k], rs_in.at[k], a_s.at[k], a_r.at[k], tdev[k]).wait_recv()
        mixed = mixed + rs_in[k].astype(jnp.float32)
    total = (total + mixed).astype(jnp.bfloat16)
    after[...] = total
    xg[z, c, x] = rms_scale(total, gain_ref[...]).astype(jnp.bfloat16)

    def zi(k):
        return (z - k + nz) % nz

    def xi(j):
        return (x - j + nx) % nx

    def gather_step(k):
        slot = xg.at[zi(k), c, x]
        if k == 0:
            for kk in range(1, nz):
                start(slot, slot, bz_s.at[kk], bz_r.at[kk], zdev[kk])
        else:
            remote(slot, slot, bz_s.at[k], bz_r.at[k], zdev[k]).wait_recv()
        for j in range(1, nx):
            start(slot, slot, bx_s.at[k, j], bx_r.at[k, j], xdev[j])
        start(slot, slot, bc_s.at[k, 0], bc_r.at[k, 0], partner)

    def cross_step(k):
        for j in range(1, nx):
            slot = xg.at[zi(k), c, xi(j)]
            remote(slot, slot, bx_s.at[k, j], bx_r.at[k, j], xdev[j]).wait_recv()
            start(slot, slot, bc_s.at[k, j], bc_r.at[k, j], partner)
        for j in range(nx):
            slot = xg.at[zi(k), 1 - c, xi(j)]
            remote(slot, slot, bc_s.at[k, j], bc_r.at[k, j], partner).wait_recv()

    def compute_step(k):
        tokens = xg[zi(k)].reshape(tp * rows, width)
        projected = jnp.dot(tokens, up_out[...].reshape(width, units), preferred_element_type=jnp.float32)
        hidden = jnp.square(jnp.maximum(projected, 0.0)).astype(jnp.bfloat16)
        cols = dn_out.shape[2]
        for b in range(dn_out.shape[0]):
            block = jnp.dot(hidden, dn_out[b], preferred_element_type=jnp.float32)
            pbuf[k, :, :, :, b * cols : (b + 1) * cols] = block.astype(jnp.bfloat16).reshape(
                CORES, nx, rows, cols
            )
        start(pbuf.at[k, 1 - c], cbuf.at[k], cc_s.at[k], cc_r.at[k], partner)

    def core_sum(k):
        remote(cbuf.at[k], cbuf.at[k], cc_s.at[k], cc_r.at[k], partner).wait_recv()
        pbuf[k, c] = (
            pbuf[k, c].astype(jnp.float32) + cbuf[k].astype(jnp.float32)
        ).astype(jnp.bfloat16)
        for j in range(1, nx):
            start(pbuf.at[k, c, (x + j) % nx], xbuf.at[k, j], cx_s.at[k, j], cx_r.at[k, j], xdev[j])

    def cross_sum(k):
        summed = pbuf[k, c, x].astype(jnp.float32)
        for j in range(1, nx):
            remote(xbuf.at[k, j], xbuf.at[k, j], cx_s.at[k, j], cx_r.at[k, j], xdev[j]).wait_recv()
            summed = summed + xbuf[k, j].astype(jnp.float32)
        zsend[k] = summed.astype(jnp.bfloat16)
        if k:
            start(zsend.at[k], zbuf.at[k], cz_s.at[k], cz_r.at[k], zback[k])

    def weights_here():
        for k in range(nz):
            for j in range(1, ny):
                for out, sy, ry in ((up_out, uy_s, uy_r), (dn_out, dy_s, dy_r)):
                    slot = out.at[block(k, j)]
                    remote(slot, slot, sy.at[k, j], ry.at[k, j], ydev[j]).wait_recv()

    gather_step(0)
    if nz > 2:
        forward(nz - 1)
    for k in range(nz):
        if k + 1 < nz:
            gather_step(k + 1)
        cross_step(k)
        if k == 0:
            weights_here()
        compute_step(k)
        if k >= 2:
            core_sum(k - 1)
        if k >= 3:
            cross_sum(k - 2)
    if nz > 1:
        core_sum(nz - 1)
    core_sum(0)
    for k in range(max(nz - 2, 1), nz):
        cross_sum(k)
    cross_sum(0)
    final = after[...].astype(jnp.float32)
    ffn = zsend[0].astype(jnp.float32)
    for k in range(1, nz):
        remote(zbuf.at[k], zbuf.at[k], cz_s.at[k], cz_r.at[k], zback[k]).wait_recv()
        ffn = ffn + zbuf[k].astype(jnp.float32)
    out_ref[...] = (final + ffn).astype(jnp.bfloat16)
    for copy in sent:
        copy.wait_send()


def layer(ny, nz, nx, latents, q_all, wks, wkl, wos, wol, resid, gain, w_up, w_down):
    tp, sp = nx * CORES, ny * nz
    rows, width = resid.shape
    tok_rows = latents.shape[0]
    heads = q_all.shape[0]
    units = w_up.shape[1] // nz
    dma = pltpu.SemaphoreType.DMA
    vmem = pl.BlockSpec(memory_space=pltpu.VMEM)
    b16 = jnp.bfloat16

    def pair(*shape):
        return [dma(shape), dma(shape)]

    return pl.pallas_call(
        functools.partial(layer_kernel, ny, nz, nx),
        out_shape=jax.ShapeDtypeStruct((rows, width), b16),
        in_specs=[vmem] * 10,
        out_specs=vmem,
        scratch_shapes=[
            pltpu.VMEM((sp,) + latents.shape, b16),
            pltpu.VMEM((sp, w_up.shape[0], units), b16),
            pltpu.VMEM((sp, units, w_down.shape[1]), b16),
            pltpu.VMEM((heads, tok_rows, 1), jnp.float32),
            pltpu.VMEM((heads, tok_rows, 1), jnp.float32),
            pltpu.VMEM((heads, tok_rows, LARGE_DIM), jnp.float32),
            pltpu.VMEM((tp, rows, width), b16),
            pltpu.VMEM((tp, rows, width), b16),
            pltpu.VMEM((rows, width), b16),
            pltpu.VMEM((nz, CORES, nx, rows, width), b16),
            pltpu.VMEM((nz, CORES, nx, rows, width), b16),
            pltpu.VMEM((nz, nx, rows, width), b16),
            pltpu.VMEM((nz, nx, rows, width), b16),
            pltpu.VMEM((nz, rows, width), b16),
            pltpu.VMEM((nz, rows, width), b16),
            dma((3,)),
        ]
        + pair(nz)
        + pair(nz, ny) * 2
        + (pair(nz) + pair(nz, ny)) * 2
        + pair(tp)
        + pair(nz)
        + pair(nz, nx)
        + pair(nz, nx)
        + pair(nz)
        + pair(nz, nx)
        + pair(nz),
        compiler_params=pltpu.CompilerParams(
            collective_id=1, has_side_effects=True, vmem_limit_bytes=63 * 2**20
        ),
        name="layer",
    )(latents, q_all, wks, wkl, wos, wol, resid, gain, w_up, w_down)


def on_device(
    ny,
    nz,
    nx,
    resid,
    q_latent,
    kv_latent,
    rope_key,
    q_gain,
    kv_gain,
    w_q_small,
    w_q_large,
    w_kv_small,
    w_kv_large,
    w_out_small,
    w_out_large,
    ffn_gain,
    w_up,
    w_down,
):
    tok_rows = q_latent.shape[0]
    offset = lax.axis_index("sp") * tok_rows
    positions = offset + jnp.arange(tok_rows, dtype=jnp.int32)
    query_normed = rms_scale(q_latent, q_gain).astype(jnp.bfloat16)
    query_small = queries(query_normed, w_q_small, SMALL_DIM, positions)
    query_large = queries(query_normed, w_q_large, LARGE_DIM, positions)
    key_normed = rms_scale(kv_latent, kv_gain).astype(jnp.bfloat16)
    key_rotated = rotary(rope_key.astype(jnp.float32), positions).astype(jnp.bfloat16)
    rope_pad = ((0, 0), (0, LANES - ROPE_DIM))
    latents = jnp.concatenate([key_normed, jnp.pad(key_rotated, rope_pad)], axis=1)

    def head_rows(query, nope_dim):
        content = jnp.pad(query[..., :nope_dim], ((0, 0), (0, 0), (0, LARGE_DIM - nope_dim)))
        turned = jnp.pad(query[..., nope_dim:], ((0, 0),) + rope_pad)
        return jnp.transpose(jnp.concatenate([content, turned], axis=-1), (1, 0, 2))

    q_all = jnp.concatenate(
        [head_rows(query_small, SMALL_DIM), head_rows(query_large, LARGE_DIM)], axis=0
    )
    return layer(
        ny,
        nz,
        nx,
        latents,
        q_all,
        w_kv_small,
        w_kv_large,
        w_out_small,
        w_out_large,
        resid,
        ffn_gain.reshape(1, -1),
        w_up,
        w_down,
    )


def solution(mesh):
    ny = inner_split(mesh.shape["sp"])
    nz = mesh.shape["sp"] // ny
    nx = mesh.shape["tp"] // CORES
    return jax.shard_map(
        functools.partial(on_device, ny, nz, nx),
        mesh=mesh,
        in_specs=(
            P(("sp", "tp"), None),
            P("sp", None),
            P("sp", None),
            P("sp", None),
            P(),
            P(),
            P(None, "tp"),
            P(None, "tp"),
            P(None, "tp"),
            P(None, "tp"),
            P("tp", None),
            P("tp", None),
            P(),
            P("sp", "tp"),
            P("tp", "sp"),
        ),
        out_specs=P(("sp", "tp"), None),
        check_vma=False,
    )
```
